32 devices in a mesh: grp: 2 (over y), sp: 4 (over z), tp: 4 (over x, core).
Axes of the slice: x: 2, y: 2, z: 4, core: 2. Of those that a mesh axis runs over, the one named last changes fastest.
Arguments:
- tokens_in: bfloat16 [2048, 2048], P(('grp', 'sp'), 'tp'), parts along dimension 0, may hold values from -6 to 6
- norm_gain: float32 [3, 2048], replicated, may hold values from 0.1 to 1.9
- w_pool_in: bfloat16 [3, 2048, 1024], P(None, 'sp', 'tp'), may hold values from -0.125 to 0.125
- w_gate: bfloat16 [3, 2048, 2048], P(None, 'sp', 'tp'), may hold values from -0.125 to 0.125
- w_back: bfloat16 [3, 1024, 2048], P(None, 'tp', 'sp'), may hold values from -0.25 to 0.25
Outputs:
- tokens_out: bfloat16 [2048, 2048], P(('grp', 'sp'), 'tp'), parts along dimension 0
The draws below stay inside these ranges and needn't reach their ends.
There are 2 independent parts, one for each index of `grp`. The reference program is written for one: setup_inputs(seed, part) draws one part's arguments, and reference() takes and returns one part's arrays. A program takes and returns all parts, laid end to end along the dimension named above; an argument that names none is the same for every part. Nothing has to cross between parts.
All inputs are finite; a program needn't handle non-finite values.
Results may differ from the reference program's by a relative error of at most 0.017.
Values may be sent and summed in bfloat16 or wider, within the bound.
A program may use at most 64 MiB of HBM per device.

```python
import jax
import jax.numpy as jnp
from jax import lax

D = 2048
POOL_WIDTH = 1024
GROUPS = 4
GRID_W = 32
LAYERS = 3
TOKENS = 1024
N_TP = 4


def spiked(drawn, key, source, target, blocks, factor):
    def block_of(axis_at):
        return (jnp.arange(drawn.shape[axis_at]) // (drawn.shape[axis_at] // blocks)).reshape((-1,) + (1,) * (drawn.ndim - 1 - axis_at))

    near = jax.random.permutation(key, blocks)[block_of(target)]
    second = (block_of(target) + blocks // 2) % blocks
    return jnp.where((block_of(source) == near) | (block_of(source) == second), factor * drawn, drawn)


def shard_levels(own_key, shape, shards, smallest, top_value):
    loudness = 1.0
    for axis_at, shards_of in shards:
        heights = jax.random.uniform(jax.random.fold_in(jax.random.fold_in(own_key, 6), axis_at), (shards_of,), jnp.float32, smallest / len(shards), top_value / len(shards))
        loudness = loudness * jnp.repeat(jnp.exp(heights), shape[axis_at] // shards_of).reshape((-1,) + (1,) * (len(shape) - 1 - axis_at))
    return loudness


def normal_values(rng, dims, deviation, most, cuts=(), kind=jnp.bfloat16):
    array = jax.random.normal(rng, dims, jnp.float32) * deviation
    if len(cuts) > 0:
        array = shard_levels(rng, dims, cuts, -0.22, 0.18) * array
    return jnp.clip(array, min=-most, max=most).astype(kind)


def heavy_noise(stream_key, extent, width, bound, cuts, heavy, kind=jnp.bfloat16):
    drawn = width * jax.random.normal(stream_key, extent, jnp.float32)
    if cuts:
        drawn = drawn * shard_levels(stream_key, extent, cuts, -0.22, 0.18)
    return jnp.clip(spiked(drawn, jax.random.fold_in(stream_key, 3), *heavy), -bound, bound).astype(kind)


def setup_inputs(seed: int = 0, part: int = 0) -> dict:
    arg_keys = jax.random.split(jax.random.key(seed), 6)
    part_splits = jax.random.split(jax.random.fold_in(arg_keys[5], part), 6)
    return {
        "tokens_in": normal_values(part_splits[0], (TOKENS, D), 1.0, 6.0, ((0, 4), (1, 4))),
        "norm_gain": jnp.clip(1.0 + 0.18 * jax.random.normal(arg_keys[1], (LAYERS, D), jnp.float32), 0.1, 1.9),
        "w_pool_in": normal_values(arg_keys[2], (LAYERS, D, POOL_WIDTH), D ** -0.5, 0.125, ((1, 4), (2, 4))),
        "w_gate": normal_values(arg_keys[3], (LAYERS, D, D), D ** -0.5, 0.125, ((1, 4), (2, 4))),
        "w_back": heavy_noise(arg_keys[4], (LAYERS, POOL_WIDTH, D), POOL_WIDTH ** -0.5, 0.25, ((1, 4), (2, 4)), (1, 2, 4, 2.0)),
    }


pool_windows = (2, 4, 8, 16)
norm_eps = 1e-06

def window_means(padded, rows_here, first_row, total_rows, window):
    reach = max(pool_windows) // 2
    half_span = window // 2
    width_cols = padded.shape[1] - 2 * reach
    row_sums = padded[reach - half_span:reach - half_span + rows_here]
    for offset in range(1 - half_span, half_span):
        row_sums = row_sums + padded[reach + offset:reach + offset + rows_here]
    box_sums = row_sums[:, reach - half_span:reach - half_span + width_cols]
    for offset in range(1 - half_span, half_span):
        box_sums = box_sums + row_sums[:, reach + offset:reach + offset + width_cols]
    row_index = first_row + jnp.arange(rows_here, dtype=jnp.int32)
    col_index = jnp.arange(width_cols, dtype=jnp.int32)
    row_counts = jnp.minimum(row_index + half_span, total_rows) - jnp.maximum(row_index - half_span, 0)
    col_counts = jnp.minimum(col_index + half_span, width_cols) - jnp.maximum(col_index - half_span, 0)
    counts = (row_counts[:, None] * col_counts[None, :]).astype(jnp.float32)
    return box_sums / counts[:, :, None]

def reference(tokens_in, norm_gain, w_pool_in, w_gate, w_back):
    reach = max(pool_windows) // 2
    group_width = POOL_WIDTH // GROUPS
    total_rows = TOKENS // GRID_W
    block_width = POOL_WIDTH // N_TP
    state = tokens_in
    for layer_id in range(LAYERS):
        wide = state.astype(jnp.float32)
        normed = (wide * lax.rsqrt(lax.optimization_barrier(jnp.mean(wide * wide, axis=-1, keepdims=True)) + norm_eps) * norm_gain[layer_id]).astype(jnp.bfloat16)
        pool_in = jnp.dot(normed, w_pool_in[layer_id], preferred_element_type=jnp.float32).astype(jnp.bfloat16)
        gate = jax.nn.sigmoid(jnp.dot(normed, w_gate[layer_id], preferred_element_type=jnp.float32))
        cells = pool_in.astype(jnp.float32).reshape(total_rows, GRID_W, POOL_WIDTH)
        padded = jnp.pad(cells, ((reach, reach), (reach, reach), (0, 0)))
        pieces = []
        for group_id in range(GROUPS):
            chosen = padded[:, :, group_id * group_width:(group_id + 1) * group_width]
            pieces.append(window_means(chosen, total_rows, 0, total_rows, pool_windows[group_id]))
        means = jnp.concatenate(pieces, axis=2)
        pooled = (means - cells).reshape(TOKENS, POOL_WIDTH).astype(jnp.bfloat16)
        branch = jnp.zeros((TOKENS, D), jnp.float32)
        for block_id in range(N_TP):
            lower = block_id * block_width
            partial_value = jnp.dot(pooled[:, lower:lower + block_width], w_back[layer_id][lower:lower + block_width], preferred_element_type=jnp.float32).astype(jnp.bfloat16)
            branch = branch + lax.optimization_barrier(partial_value).astype(jnp.float32)
        state = (wide + gate * branch).astype(jnp.bfloat16)
    return state
```

```python
import jax
import jax.numpy as jnp
from jax import lax
from jax.experimental import pallas as pl
from jax.experimental.pallas import tpu as pltpu
from jax.sharding import PartitionSpec as P
import functools

POOL_WIDTH = 1024
GROUPS = 4
GRID_W = 32
LAYERS = 3


pool_windows = (2, 4, 8, 16)
norm_eps = 1e-06


def padded_2(value, sides, width):
    for axis, dim in sides:
        peers, length = (lax.axis_size(axis), value.shape[dim])
        up = [(i, (i + 1) % peers) for i in range(peers - 1)]
        down = [(j, i) for i, j in up]
        last = lax.slice_in_dim(value, length - width, length, axis=dim)
        initial = lax.slice_in_dim(value, 0, width, axis=dim)
        before = lax.ppermute(last, axis, up)
        after = lax.ppermute(initial, axis, down)
        value = jnp.concatenate([before, value, after], axis=dim)
    return value


def window_means(padded, rows_here, first_row, total_rows, window):
    reach = max(pool_windows) // 2
    half_span = window // 2
    width_cols = padded.shape[1] - 2 * reach
    row_sums = padded[reach - half_span : reach - half_span + rows_here]
    for offset in range(1 - half_span, half_span):
        row_sums = row_sums + padded[reach + offset : reach + offset + rows_here]
    box_sums = row_sums[:, reach - half_span : reach - half_span + width_cols]
    for offset in range(1 - half_span, half_span):
        box_sums = box_sums + row_sums[:, reach + offset : reach + offset + width_cols]
    row_index = first_row + jnp.arange(rows_here, dtype=jnp.int32)
    col_index = jnp.arange(width_cols, dtype=jnp.int32)
    row_counts = jnp.minimum(row_index + half_span, total_rows) - jnp.maximum(
        row_index - half_span, 0
    )
    col_counts = jnp.minimum(col_index + half_span, width_cols) - jnp.maximum(
        col_index - half_span, 0
    )
    counts = (row_counts[:, None] * col_counts[None, :]).astype(jnp.float32)
    return box_sums / counts[:, :, None]


def on_device(tokens_in, norm_gain, w_pool_in, w_gate, w_back):
    reach = max(pool_windows) // 2
    sp_count = lax.axis_size("sp")
    tp_count = lax.axis_size("tp")
    tp_pos = lax.axis_index("tp")
    sp_pos = lax.axis_index("sp")
    tok_rows = tokens_in.shape[0]
    rows_here = tok_rows // GRID_W
    total_rows = rows_here * sp_count
    first_row = sp_pos * rows_here
    local_pool = w_pool_in.shape[2]
    group_width = POOL_WIDTH // GROUPS
    channel_group = (tp_pos * local_pool + jnp.arange(local_pool, dtype=jnp.int32)) // group_width
    state = tokens_in
    for layer_id in range(LAYERS):
        whole_rows = lax.all_gather(state, "tp", axis=1, tiled=True)
        wide = whole_rows.astype(jnp.float32)
        normed = (
            wide
            * lax.rsqrt(jnp.mean(wide * wide, axis=-1, keepdims=True) + norm_eps)
            * norm_gain[layer_id]
        ).astype(jnp.bfloat16)
        pool_acc = jnp.dot(
            normed,
            lax.all_gather(w_pool_in[layer_id], "sp", axis=0, tiled=True),
            preferred_element_type=jnp.float32,
        )
        gate_acc = jnp.dot(
            normed,
            lax.all_gather(w_gate[layer_id], "sp", axis=0, tiled=True),
            preferred_element_type=jnp.float32,
        )
        pool_in = pool_acc.astype(jnp.bfloat16)
        gate = jax.nn.sigmoid(gate_acc)
        cells = pool_in.reshape(rows_here, GRID_W, local_pool)
        rimmed = padded_2(cells, (("sp", 0),), reach)
        padded = jnp.pad(rimmed.astype(jnp.float32), ((0, 0), (reach, reach), (0, 0)))
        means = jnp.zeros((rows_here, GRID_W, local_pool), jnp.float32)
        for group_id in range(GROUPS):
            in_group = (channel_group == group_id)[None, None, :]
            means = jnp.where(
                in_group,
                window_means(padded, rows_here, first_row, total_rows, pool_windows[group_id]),
                means,
            )
        pooled = (
            (means - cells.astype(jnp.float32)).reshape(tok_rows, local_pool).astype(jnp.bfloat16)
        )
        full_pooled = lax.all_gather(pooled, "tp", axis=1, tiled=True)
        back_rows = lax.all_gather(w_back[layer_id], "sp", axis=1, tiled=True)
        back_cols = lax.all_to_all(back_rows, "tp", split_axis=1, concat_axis=0, tiled=True)
        partials = jnp.einsum(
            "tnb,nbd->ntd",
            full_pooled.reshape(tok_rows, tp_count, local_pool),
            back_cols.reshape(tp_count, local_pool, back_cols.shape[1]),
            preferred_element_type=jnp.float32,
        ).astype(jnp.bfloat16)
        branch = jnp.sum(partials.astype(jnp.float32), axis=0)
        state = (state.astype(jnp.float32) + gate * branch).astype(jnp.bfloat16)
    return state


MESH = pl.DeviceIdType.MESH


def halves(buffers, layer, block, half):
    views = []
    for buf in buffers:
        rows = buf.shape[2] // 2
        views.append(buf.at[layer, block, pl.ds(pl.multiple_of(half * rows, rows), rows), :])
    return views


def fused_kernel(
    sp_count, tp_count,
    tok_hbm, gain_ref, wp_hbm, wg_hbm, wb_hbm, out_ref,
    wp, wg, wb, gathered, normed, halo, gate_buf, box, counts, parts, arrived,
    load_sem, z_send, z_recv, y_send, y_recv, ag_send, ag_recv, h_send, h_recv, rs_send, rs_recv,
):
    g = lax.axis_index("grp")
    s = lax.axis_index("sp")
    t = lax.axis_index("tp")
    other = 1 - g
    t1 = t + 1 - 2 * (t % 2)
    t2 = (t + 2) % tp_count
    t3 = (t1 + 2) % tp_count
    last = sp_count - 1
    toks, feats = tok_hbm.shape
    rows_here = toks // GRID_W
    total_rows = rows_here * sp_count
    weights = (wp, wg, wb)
    sources = (wp_hbm, wg_hbm, wb_hbm)
    rounds = sp_count - 1

    def load(layer, piece):
        return pltpu.make_async_copy(
            sources[piece].at[layer], weights[piece].at[layer, s], load_sem.at[layer, piece]
        )

    state_load = pltpu.make_async_copy(tok_hbm, gathered.at[0, t], load_sem.at[LAYERS, 0])
    state_load.start()
    for piece in range(3):
        load(0, piece).start()
    for layer in range(1, LAYERS):
        for piece in range(3):
            load(layer, piece).start()

    barrier = pltpu.get_barrier_semaphore()
    for target in ({"grp": other}, {"tp": t1}, {"tp": t2}, {"tp": t3}):
        pl.semaphore_signal(barrier, inc=1, device_id=target, device_id_type=MESH)

    @pl.when(s > 0)
    def _():
        pl.semaphore_signal(barrier, inc=1, device_id={"sp": s - 1}, device_id_type=MESH)

    @pl.when(s < last)
    def _():
        pl.semaphore_signal(barrier, inc=1, device_id={"sp": s + 1}, device_id_type=MESH)

    pl.semaphore_wait(barrier, 4 + jnp.where(s > 0, 1, 0) + jnp.where(s < last, 1, 0))

    def sent_block(way, k):
        return s - k if way == 0 else s + k

    def got_block(way, k):
        return s - 1 - k if way == 0 else s + 1 + k

    def gets(way, k):
        return s - 1 - k >= 0 if way == 0 else s + 1 + k <= last

    def sends(way, k):
        if way == 0:
            return jnp.logical_and(s - k >= 0, s < last)
        return jnp.logical_and(s + k <= last, s > 0)

    def z_copy(layer, way, k, piece, block):
        view = halves(weights, layer, block, g)[piece]
        return pltpu.make_async_remote_copy(
            src_ref=view, dst_ref=view,
            send_sem=z_send.at[layer, way, k, piece], recv_sem=z_recv.at[layer, way, k, piece],
            device_id={"sp": s + 1 if way == 0 else s - 1}, device_id_type=MESH,
        )

    def y_copy(layer, way, k, piece, half):
        view = halves(weights, layer, got_block(way, k), half)[piece]
        return pltpu.make_async_remote_copy(
            src_ref=view, dst_ref=view,
            send_sem=y_send.at[layer, way, k, piece], recv_sem=y_recv.at[layer, way, k, piece],
            device_id={"grp": other}, device_id_type=MESH,
        )

    def own_sends(layer):
        for piece in range(3):
            load(layer, piece).wait()
            for way in range(2):
                @pl.when(sends(way, 0))
                def _(way=way, piece=piece):
                    z_copy(layer, way, 0, piece, s).start()

    def pump(layer, k):
        for piece in range(3):
            for way in range(2):
                @pl.when(gets(way, k))
                def _(way=way, piece=piece):
                    z_copy(layer, way, k, piece, got_block(way, k)).wait_recv()
                    y_copy(layer, way, k, piece, g).start()
                if k + 1 < rounds:
                    @pl.when(sends(way, k + 1))
                    def _(way=way, piece=piece):
                        z_copy(layer, way, k + 1, piece, sent_block(way, k + 1)).start()

    def await_y(layer, piece):
        for k in range(rounds):
            for way in range(2):
                @pl.when(gets(way, k))
                def _(way=way, k=k):
                    y_copy(layer, way, k, piece, other).wait_recv()

    def ag_copy(layer, which, block, target):
        return pltpu.make_async_remote_copy(
            src_ref=gathered.at[layer, block], dst_ref=gathered.at[layer, block],
            send_sem=ag_send.at[layer, which], recv_sem=ag_recv.at[layer, which],
            device_id={"tp": target}, device_id_type=MESH,
        )

    def start_gather(layer):
        ag_copy(layer, 0, t, t2).start()
        ag_copy(layer, 1, t, t1).start()

    def h_copy(layer, way):
        return pltpu.make_async_remote_copy(
            src_ref=halo.at[layer, 1], dst_ref=halo.at[layer, 0 if way == 0 else 2],
            send_sem=h_send.at[layer, way], recv_sem=h_recv.at[layer, way],
            device_id={"sp": s + 1 if way == 0 else s - 1}, device_id_type=MESH,
        )

    def rs_copy(layer, which, target):
        return pltpu.make_async_remote_copy(
            src_ref=parts.at[layer, target], dst_ref=arrived.at[layer, which],
            send_sem=rs_send.at[layer, which], recv_sem=rs_recv.at[layer, which],
            device_id={"tp": target}, device_id_type=MESH,
        )

    state_load.wait()
    start_gather(0)
    own_sends(0)

    half_span = jnp.int32(pool_windows[0] // 2)
    for group_id in range(1, GROUPS):
        half_span = jnp.where(t == group_id, pool_windows[group_id] // 2, half_span)
    shift = GRID_W.bit_length() - 1
    first_row = s * rows_here
    out_tok = lax.broadcasted_iota(jnp.int32, (toks, toks), 0)
    in_tok = lax.broadcasted_iota(jnp.int32, (toks, toks), 1)
    out_row = first_row + lax.shift_right_logical(out_tok, shift)
    out_col = lax.bitwise_and(out_tok, GRID_W - 1)
    in_col = lax.bitwise_and(in_tok, GRID_W - 1)
    near_col = (in_col >= out_col - half_span) & (in_col < out_col + half_span)
    for slot in range(3):
        in_row = first_row + (slot - 1) * rows_here + lax.shift_right_logical(in_tok, shift)
        inside = (
            near_col
            & (in_row >= out_row - half_span) & (in_row < out_row + half_span)
            & (in_row >= 0) & (in_row < total_rows)
        )
        box[slot] = jnp.where(inside, 1.0, 0.0).astype(jnp.bfloat16)
    tok_at = lax.broadcasted_iota(jnp.int32, counts.shape, 0)
    row_at = first_row + lax.shift_right_logical(tok_at, shift)
    col_at = lax.bitwise_and(tok_at, GRID_W - 1)
    row_counts = jnp.minimum(row_at + half_span, total_rows) - jnp.maximum(row_at - half_span, 0)
    col_counts = jnp.minimum(col_at + half_span, GRID_W) - jnp.maximum(col_at - half_span, 0)
    counts[...] = (row_counts * col_counts).astype(jnp.float32)

    @pl.when(s == 0)
    def _():
        for layer in range(LAYERS):
            halo[layer, 0] = jnp.zeros(halo.shape[2:], halo.dtype)

    @pl.when(s == last)
    def _():
        for layer in range(LAYERS):
            halo[layer, 2] = jnp.zeros(halo.shape[2:], halo.dtype)

    for k in range(rounds):
        pump(0, k)

    def one_layer(layer, _):
        more = layer + 1 < LAYERS

        @pl.when(more)
        def _():
            own_sends(layer + 1)

        ag_copy(layer, 0, t2, t2).wait_recv()
        ag_copy(layer, 2, t2, t1).start()
        ag_copy(layer, 1, t1, t1).wait_recv()
        ag_copy(layer, 2, t3, t1).wait_recv()
        total = jnp.zeros((toks, 1), jnp.float32)
        for block in range(tp_count):
            wide = gathered[layer, block].astype(jnp.float32)
            total = total + jnp.sum(wide * wide, axis=1, keepdims=True)
        scale = lax.rsqrt(total / (tp_count * feats) + norm_eps)
        for block in range(tp_count):
            cols = slice(block * feats, (block + 1) * feats)
            wide = gathered[layer, block].astype(jnp.float32)
            normed[:, cols] = (wide * scale * gain_ref[pl.ds(layer, 1), cols]).astype(jnp.bfloat16)

        @pl.when(more)
        def _():
            pump(layer + 1, 0)

        depth = wp.shape[2]

        def project(buf):
            acc = None
            for block in range(sp_count):
                term = jnp.dot(
                    normed[:, block * depth:(block + 1) * depth], buf[layer, block],
                    preferred_element_type=jnp.float32,
                )
                acc = term if acc is None else acc + term
            return acc

        await_y(layer, 0)
        halo[layer, 1] = project(wp).astype(jnp.bfloat16)

        @pl.when(s < last)
        def _():
            h_copy(layer, 0).start()

        @pl.when(s > 0)
        def _():
            h_copy(layer, 1).start()

        await_y(layer, 1)
        gate_buf[...] = jax.nn.sigmoid(project(wg))

        @pl.when(more)
        def _():
            pump(layer + 1, 1)

        @pl.when(s > 0)
        def _():
            h_copy(layer, 0).wait_recv()

        @pl.when(s < last)
        def _():
            h_copy(layer, 1).wait_recv()

        sums = jnp.zeros(counts.shape, jnp.float32)
        for slot in range(3):
            sums = sums + jnp.dot(box[slot], halo[layer, slot], preferred_element_type=jnp.float32)
        pooled = (sums / counts[...] - halo[layer, 1].astype(jnp.float32)).astype(jnp.bfloat16)
        await_y(layer, 2)
        for which, target in ((1, t3), (0, t2), (2, t1), (None, t)):
            parts[layer, target] = jnp.dot(
                pooled, wb[layer, target], preferred_element_type=jnp.float32
            ).astype(jnp.bfloat16)
            if which is not None:
                rs_copy(layer, which, target).start()

        @pl.when(more)
        def _():
            pump(layer + 1, 2)

        branch = parts[layer, t].astype(jnp.float32)
        for which in (2, 0, 1):
            rs_copy(layer, which, t1).wait_recv()
            branch = branch + arrived[layer, which].astype(jnp.float32)
        state = (gathered[layer, t].astype(jnp.float32) + gate_buf[...] * branch).astype(jnp.bfloat16)

        @pl.when(more)
        def _():
            gathered[layer + 1, t] = state
            start_gather(layer + 1)

        @pl.when(layer + 1 == LAYERS)
        def _():
            out_ref[...] = state

        return 0

    lax.fori_loop(0, LAYERS, one_layer, 0)

    def drain(layer, _):
        for piece in range(3):
            for k in range(rounds):
                for way in range(2):
                    @pl.when(sends(way, k))
                    def _(way=way, k=k, piece=piece):
                        z_copy(layer, way, k, piece, sent_block(way, k)).wait_send()

                    @pl.when(gets(way, k))
                    def _(way=way, k=k, piece=piece):
                        y_copy(layer, way, k, piece, g).wait_send()
        ag_copy(layer, 0, t, t2).wait_send()
        ag_copy(layer, 1, t, t1).wait_send()
        ag_copy(layer, 2, t2, t1).wait_send()

        @pl.when(s < last)
        def _():
            h_copy(layer, 0).wait_send()

        @pl.when(s > 0)
        def _():
            h_copy(layer, 1).wait_send()

        rs_copy(layer, 0, t2).wait_send()
        rs_copy(layer, 1, t3).wait_send()
        rs_copy(layer, 2, t1).wait_send()
        return 0

    lax.fori_loop(0, LAYERS, drain, 0)


def fused(tokens_in, norm_gain, w_pool_in, w_gate, w_back):
    sp_count, tp_count = lax.axis_size("sp"), lax.axis_size("tp")
    toks, feats = tokens_in.shape
    _, depth, local_pool = w_pool_in.shape
    rounds = sp_count - 1
    bf, f32 = jnp.bfloat16, jnp.float32
    dma = pltpu.SemaphoreType.DMA
    streams = dma((LAYERS, 2, rounds, 3))
    return pl.pallas_call(
        functools.partial(fused_kernel, sp_count, tp_count),
        out_shape=jax.ShapeDtypeStruct((toks, feats), bf),
        in_specs=[
            pl.BlockSpec(memory_space=pltpu.HBM),
            pl.BlockSpec(memory_space=pltpu.VMEM),
            pl.BlockSpec(memory_space=pltpu.HBM),
            pl.BlockSpec(memory_space=pltpu.HBM),
            pl.BlockSpec(memory_space=pltpu.HBM),
        ],
        out_specs=pl.BlockSpec(memory_space=pltpu.VMEM),
        scratch_shapes=[
            pltpu.VMEM((LAYERS, sp_count) + w_pool_in.shape[1:], bf),
            pltpu.VMEM((LAYERS, sp_count) + w_gate.shape[1:], bf),
            pltpu.VMEM((LAYERS, sp_count) + w_back.shape[1:], bf),
            pltpu.VMEM((LAYERS, tp_count, toks, feats), bf),
            pltpu.VMEM((toks, tp_count * feats), bf),
            pltpu.VMEM((LAYERS, 3, toks, local_pool), bf),
            pltpu.VMEM((toks, feats), f32),
            pltpu.VMEM((3, toks, toks), bf),
            pltpu.VMEM((toks, local_pool), f32),
            pltpu.VMEM((LAYERS, tp_count, toks, feats), bf),
            pltpu.VMEM((LAYERS, 3, toks, feats), bf),
            dma((LAYERS + 1, 3)),
            streams, streams, streams, streams,
            dma((LAYERS, 3)), dma((LAYERS, 3)),
            dma((LAYERS, 2)), dma((LAYERS, 2)),
            dma((LAYERS, 3)), dma((LAYERS, 3)),
        ],
        compiler_params=pltpu.CompilerParams(
            collective_id=0, has_side_effects=True, vmem_limit_bytes=56 * 1024 * 1024
        ),
    )(tokens_in, norm_gain, w_pool_in, w_gate, w_back)


def dispatch(tokens_in, norm_gain, w_pool_in, w_gate, w_back):
    fits = (
        lax.axis_size("grp") == 2
        and lax.axis_size("tp") == GROUPS == 4
        and lax.axis_size("sp") == lax.axis_size("tp")
        and w_pool_in.shape[2] * GROUPS == POOL_WIDTH
        and w_pool_in.shape[1] == tokens_in.shape[1]
        and tokens_in.shape[0] // GRID_W >= max(pool_windows) // 2
    )
    step = fused if fits else on_device
    return step(tokens_in, norm_gain, w_pool_in, w_gate, w_back)


def solution(mesh):
    return jax.shard_map(
        dispatch,
        mesh=mesh,
        in_specs=(
            P(("grp", "sp"), "tp"),
            P(),
            P(None, "sp", "tp"),
            P(None, "sp", "tp"),
            P(None, "tp", "sp"),
        ),
        out_specs=P(("grp", "sp"), "tp"),
        check_vma=False,
    )
```

```python
import jax
import jax.numpy as jnp
from jax import lax
from jax.experimental import pallas as pl
from jax.experimental.pallas import tpu as pltpu
from jax.sharding import PartitionSpec as P
import functools

POOL_WIDTH = 1024
GROUPS = 4
GRID_W = 32
LAYERS = 3


pool_windows = (2, 4, 8, 16)
norm_eps = 1e-06


def padded_2(value, sides, width):
    for axis, dim in sides:
        peers, length = (lax.axis_size(axis), value.shape[dim])
        up = [(i, (i + 1) % peers) for i in range(peers - 1)]
        down = [(j, i) for i, j in up]
        last = lax.slice_in_dim(value, length - width, length, axis=dim)
        initial = lax.slice_in_dim(value, 0, width, axis=dim)
        before = lax.ppermute(last, axis, up)
        after = lax.ppermute(initial, axis, down)
        value = jnp.concatenate([before, value, after], axis=dim)
    return value


def window_means(padded, rows_here, first_row, total_rows, window):
    reach = max(pool_windows) // 2
    half_span = window // 2
    width_cols = padded.shape[1] - 2 * reach
    row_sums = padded[reach - half_span : reach - half_span + rows_here]
    for offset in range(1 - half_span, half_span):
        row_sums = row_sums + padded[reach + offset : reach + offset + rows_here]
    box_sums = row_sums[:, reach - half_span : reach - half_span + width_cols]
    for offset in range(1 - half_span, half_span):
        box_sums = box_sums + row_sums[:, reach + offset : reach + offset + width_cols]
    row_index = first_row + jnp.arange(rows_here, dtype=jnp.int32)
    col_index = jnp.arange(width_cols, dtype=jnp.int32)
    row_counts = jnp.minimum(row_index + half_span, total_rows) - jnp.maximum(
        row_index - half_span, 0
    )
    col_counts = jnp.minimum(col_index + half_span, width_cols) - jnp.maximum(
        col_index - half_span, 0
    )
    counts = (row_counts[:, None] * col_counts[None, :]).astype(jnp.float32)
    return box_sums / counts[:, :, None]


def on_device(tokens_in, norm_gain, w_pool_in, w_gate, w_back):
    reach = max(pool_windows) // 2
    sp_count = lax.axis_size("sp")
    tp_count = lax.axis_size("tp")
    tp_pos = lax.axis_index("tp")
    sp_pos = lax.axis_index("sp")
    tok_rows = tokens_in.shape[0]
    rows_here = tok_rows // GRID_W
    total_rows = rows_here * sp_count
    first_row = sp_pos * rows_here
    local_pool = w_pool_in.shape[2]
    group_width = POOL_WIDTH // GROUPS
    channel_group = (tp_pos * local_pool + jnp.arange(local_pool, dtype=jnp.int32)) // group_width
    state = tokens_in
    for layer_id in range(LAYERS):
        whole_rows = lax.all_gather(state, "tp", axis=1, tiled=True)
        wide = whole_rows.astype(jnp.float32)
        normed = (
            wide
            * lax.rsqrt(jnp.mean(wide * wide, axis=-1, keepdims=True) + norm_eps)
            * norm_gain[layer_id]
        ).astype(jnp.bfloat16)
        pool_acc = jnp.dot(
            normed,
            lax.all_gather(w_pool_in[layer_id], "sp", axis=0, tiled=True),
            preferred_element_type=jnp.float32,
        )
        gate_acc = jnp.dot(
            normed,
            lax.all_gather(w_gate[layer_id], "sp", axis=0, tiled=True),
            preferred_element_type=jnp.float32,
        )
        pool_in = pool_acc.astype(jnp.bfloat16)
        gate = jax.nn.sigmoid(gate_acc)
        cells = pool_in.reshape(rows_here, GRID_W, local_pool)
        rimmed = padded_2(cells, (("sp", 0),), reach)
        padded = jnp.pad(rimmed.astype(jnp.float32), ((0, 0), (reach, reach), (0, 0)))
        means = jnp.zeros((rows_here, GRID_W, local_pool), jnp.float32)
        for group_id in range(GROUPS):
            in_group = (channel_group == group_id)[None, None, :]
            means = jnp.where(
                in_group,
                window_means(padded, rows_here, first_row, total_rows, pool_windows[group_id]),
                means,
            )
        pooled = (
            (means - cells.astype(jnp.float32)).reshape(tok_rows, local_pool).astype(jnp.bfloat16)
        )
        full_pooled = lax.all_gather(pooled, "tp", axis=1, tiled=True)
        back_rows = lax.all_gather(w_back[layer_id], "sp", axis=1, tiled=True)
        back_cols = lax.all_to_all(back_rows, "tp", split_axis=1, concat_axis=0, tiled=True)
        partials = jnp.einsum(
            "tnb,nbd->ntd",
            full_pooled.reshape(tok_rows, tp_count, local_pool),
            back_cols.reshape(tp_count, local_pool, back_cols.shape[1]),
            preferred_element_type=jnp.float32,
        ).astype(jnp.bfloat16)
        branch = jnp.sum(partials.astype(jnp.float32), axis=0)
        state = (state.astype(jnp.float32) + gate * branch).astype(jnp.bfloat16)
    return state


MESH = pl.DeviceIdType.MESH
POOL, GATE, BACK = range(3)


def halves(buffers, layer, block, half):
    views = []
    for buf in buffers:
        rows = buf.shape[2] // 2
        views.append(buf.at[layer, block, pl.ds(pl.multiple_of(half * rows, rows), rows), :])
    return views


def fused_kernel(
    sp_count, tp_count,
    tok_hbm, gain_ref, wp_hbm, wg_hbm, wb_hbm, out_ref,
    wp, wg, wb, gathered, normed, halo, gate_buf, box, counts, parts, arrived,
    load_sem, z_send, z_recv, y_send, y_recv, ag_send, ag_recv, h_send, h_recv, rs_send, rs_recv,
):
    g = lax.axis_index("grp")
    s = lax.axis_index("sp")
    t = lax.axis_index("tp")
    other = 1 - g
    t1 = t + 1 - 2 * (t % 2)
    t2 = (t + 2) % tp_count
    t3 = (t1 + 2) % tp_count
    last = sp_count - 1
    toks, feats = tok_hbm.shape
    rows_here = toks // GRID_W
    total_rows = rows_here * sp_count
    weights = (wp, wg, wb)
    sources = (wp_hbm, wg_hbm, wb_hbm)
    rounds = sp_count - 1

    def load(layer, piece):
        return pltpu.make_async_copy(
            sources[piece].at[layer], weights[piece].at[layer, s], load_sem.at[layer, piece]
        )

    state_load = pltpu.make_async_copy(tok_hbm, gathered.at[0, t], load_sem.at[LAYERS, 0])
    state_load.start()
    for piece in range(3):
        load(0, piece).start()
    for layer in range(1, LAYERS):
        for piece in range(3):
            load(layer, piece).start()

    barrier = pltpu.get_barrier_semaphore()
    for target in ({"grp": other}, {"tp": t1}, {"tp": t2}, {"tp": t3}):
        pl.semaphore_signal(barrier, inc=1, device_id=target, device_id_type=MESH)

    @pl.when(s > 0)
    def _():
        pl.semaphore_signal(barrier, inc=1, device_id={"sp": s - 1}, device_id_type=MESH)

    @pl.when(s < last)
    def _():
        pl.semaphore_signal(barrier, inc=1, device_id={"sp": s + 1}, device_id_type=MESH)

    pl.semaphore_wait(barrier, 4 + jnp.where(s > 0, 1, 0) + jnp.where(s < last, 1, 0))

    def sent_block(way, k):
        return s - k if way == 0 else s + k

    def got_block(way, k):
        return s - 1 - k if way == 0 else s + 1 + k

    def gets(way, k):
        return s - 1 - k >= 0 if way == 0 else s + 1 + k <= last

    def sends(way, k):
        if way == 0:
            return jnp.logical_and(s - k >= 0, s < last)
        return jnp.logical_and(s + k <= last, s > 0)

    def z_copy(layer, way, k, piece, block):
        view = halves(weights, layer, block, g)[piece]
        return pltpu.make_async_remote_copy(
            src_ref=view, dst_ref=view,
            send_sem=z_send.at[layer, way, k, piece], recv_sem=z_recv.at[layer, way, k, piece],
            device_id={"sp": s + 1 if way == 0 else s - 1}, device_id_type=MESH,
        )

    def y_copy(layer, way, k, piece, half):
        view = halves(weights, layer, got_block(way, k), half)[piece]
        return pltpu.make_async_remote_copy(
            src_ref=view, dst_ref=view,
            send_sem=y_send.at[layer, way, k, piece], recv_sem=y_recv.at[layer, way, k, piece],
            device_id={"grp": other}, device_id_type=MESH,
        )

    def own_sends(layer, piece):
        load(layer, piece).wait()
        for way in range(2):
            @pl.when(sends(way, 0))
            def _(way=way):
                z_copy(layer, way, 0, piece, s).start()

    def pump(layer, piece, k):
        for way in range(2):
            @pl.when(gets(way, k))
            def _(way=way):
                z_copy(layer, way, k, piece, got_block(way, k)).wait_recv()
                y_copy(layer, way, k, piece, g).start()
            if k + 1 < rounds:
                @pl.when(sends(way, k + 1))
                def _(way=way):
                    z_copy(layer, way, k + 1, piece, sent_block(way, k + 1)).start()

    def await_y(layer, piece):
        for k in range(rounds):
            for way in range(2):
                @pl.when(gets(way, k))
                def _(way=way, k=k):
                    y_copy(layer, way, k, piece, other).wait_recv()

    def ag_copy(layer, which, block, target):
        return pltpu.make_async_remote_copy(
            src_ref=gathered.at[layer, block], dst_ref=gathered.at[layer, block],
            send_sem=ag_send.at[layer, which], recv_sem=ag_recv.at[layer, which],
            device_id={"tp": target}, device_id_type=MESH,
        )

    def start_gather(layer):
        ag_copy(layer, 0, t, t2).start()
        ag_copy(layer, 1, t, t1).start()

    def h_copy(layer, way):
        return pltpu.make_async_remote_copy(
            src_ref=halo.at[layer, 1], dst_ref=halo.at[layer, 0 if way == 0 else 2],
            send_sem=h_send.at[layer, way], recv_sem=h_recv.at[layer, way],
            device_id={"sp": s + 1 if way == 0 else s - 1}, device_id_type=MESH,
        )

    def rs_copy(layer, which, target):
        return pltpu.make_async_remote_copy(
            src_ref=parts.at[layer, target], dst_ref=arrived.at[layer, which],
            send_sem=rs_send.at[layer, which], recv_sem=rs_recv.at[layer, which],
            device_id={"tp": target}, device_id_type=MESH,
        )

    state_load.wait()
    start_gather(0)
    own_sends(0, POOL)
    own_sends(0, BACK)

    half_span = jnp.int32(pool_windows[0] // 2)
    for group_id in range(1, GROUPS):
        half_span = jnp.where(t == group_id, pool_windows[group_id] // 2, half_span)
    shift = GRID_W.bit_length() - 1
    first_row = s * rows_here
    out_tok = lax.broadcasted_iota(jnp.int32, (toks, toks), 0)
    in_tok = lax.broadcasted_iota(jnp.int32, (toks, toks), 1)
    out_row = first_row + lax.shift_right_logical(out_tok, shift)
    out_col = lax.bitwise_and(out_tok, GRID_W - 1)
    in_col = lax.bitwise_and(in_tok, GRID_W - 1)
    near_col = (in_col >= out_col - half_span) & (in_col < out_col + half_span)
    for slot in range(3):
        in_row = first_row + (slot - 1) * rows_here + lax.shift_right_logical(in_tok, shift)
        inside = (
            near_col
            & (in_row >= out_row - half_span) & (in_row < out_row + half_span)
            & (in_row >= 0) & (in_row < total_rows)
        )
        box[slot] = jnp.where(inside, 1.0, 0.0).astype(jnp.bfloat16)
    tok_at = lax.broadcasted_iota(jnp.int32, counts.shape, 0)
    row_at = first_row + lax.shift_right_logical(tok_at, shift)
    col_at = lax.bitwise_and(tok_at, GRID_W - 1)
    row_counts = jnp.minimum(row_at + half_span, total_rows) - jnp.maximum(row_at - half_span, 0)
    col_counts = jnp.minimum(col_at + half_span, GRID_W) - jnp.maximum(col_at - half_span, 0)
    counts[...] = (row_counts * col_counts).astype(jnp.float32)

    @pl.when(s == 0)
    def _():
        for layer in range(LAYERS):
            halo[layer, 0] = jnp.zeros(halo.shape[2:], halo.dtype)

    @pl.when(s == last)
    def _():
        for layer in range(LAYERS):
            halo[layer, 2] = jnp.zeros(halo.shape[2:], halo.dtype)

    for k in range(rounds):
        pump(0, POOL, k)

    def one_layer(layer, _):
        more = layer + 1 < LAYERS

        own_sends(layer, GATE)
        ag_copy(layer, 0, t2, t2).wait_recv()
        ag_copy(layer, 2, t2, t1).start()
        ag_copy(layer, 1, t1, t1).wait_recv()
        ag_copy(layer, 2, t3, t1).wait_recv()
        total = jnp.zeros((toks, 1), jnp.float32)
        for block in range(tp_count):
            wide = gathered[layer, block].astype(jnp.float32)
            total = total + jnp.sum(wide * wide, axis=1, keepdims=True)
        scale = lax.rsqrt(total / (tp_count * feats) + norm_eps)
        for block in range(tp_count):
            cols = slice(block * feats, (block + 1) * feats)
            wide = gathered[layer, block].astype(jnp.float32)
            normed[:, cols] = (wide * scale * gain_ref[pl.ds(layer, 1), cols]).astype(jnp.bfloat16)

        for k in range(rounds - 1):
            pump(layer, BACK, k)
        depth = wp.shape[2]

        def project(buf):
            acc = None
            for block in range(sp_count):
                term = jnp.dot(
                    normed[:, block * depth:(block + 1) * depth], buf[layer, block],
                    preferred_element_type=jnp.float32,
                )
                acc = term if acc is None else acc + term
            return acc

        await_y(layer, POOL)
        halo[layer, 1] = project(wp).astype(jnp.bfloat16)

        @pl.when(s < last)
        def _():
            h_copy(layer, 0).start()

        @pl.when(s > 0)
        def _():
            h_copy(layer, 1).start()

        pump(layer, BACK, rounds - 1)

        @pl.when(more)
        def _():
            own_sends(layer + 1, POOL)

        pump(layer, GATE, 0)

        @pl.when(s > 0)
        def _():
            h_copy(layer, 0).wait_recv()

        @pl.when(s < last)
        def _():
            h_copy(layer, 1).wait_recv()

        sums = jnp.zeros(counts.shape, jnp.float32)
        for slot in range(3):
            sums = sums + jnp.dot(box[slot], halo[layer, slot], preferred_element_type=jnp.float32)
        pooled = (sums / counts[...] - halo[layer, 1].astype(jnp.float32)).astype(jnp.bfloat16)
        await_y(layer, BACK)
        for which, target in ((1, t3), (0, t2), (2, t1), (None, t)):
            parts[layer, target] = jnp.dot(
                pooled, wb[layer, target], preferred_element_type=jnp.float32
            ).astype(jnp.bfloat16)
            if which is not None:
                rs_copy(layer, which, target).start()

        for k in range(1, rounds):
            pump(layer, GATE, k)

        @pl.when(more)
        def _():
            own_sends(layer + 1, BACK)
            for k in range(rounds - 1):
                pump(layer + 1, POOL, k)

        await_y(layer, GATE)
        gate_buf[...] = jax.nn.sigmoid(project(wg))
        branch = parts[layer, t].astype(jnp.float32)
        for which in (2, 0, 1):
            rs_copy(layer, which, t1).wait_recv()
            branch = branch + arrived[layer, which].astype(jnp.float32)
        state = (gathered[layer, t].astype(jnp.float32) + gate_buf[...] * branch).astype(jnp.bfloat16)

        @pl.when(more)
        def _():
            gathered[layer + 1, t] = state
            start_gather(layer + 1)
            pump(layer + 1, POOL, rounds - 1)

        @pl.when(layer + 1 == LAYERS)
        def _():
            out_ref[...] = state

        return 0

    lax.fori_loop(0, LAYERS, one_layer, 0)

    def drain(layer, _):
        for piece in range(3):
            for k in range(rounds):
                for way in range(2):
                    @pl.when(sends(way, k))
                    def _(way=way, k=k, piece=piece):
                        z_copy(layer, way, k, piece, sent_block(way, k)).wait_send()

                    @pl.when(gets(way, k))
                    def _(way=way, k=k, piece=piece):
                        y_copy(layer, way, k, piece, g).wait_send()
        ag_copy(layer, 0, t, t2).wait_send()
        ag_copy(layer, 1, t, t1).wait_send()
        ag_copy(layer, 2, t2, t1).wait_send()

        @pl.when(s < last)
        def _():
            h_copy(layer, 0).wait_send()

        @pl.when(s > 0)
        def _():
            h_copy(layer, 1).wait_send()

        rs_copy(layer, 0, t2).wait_send()
        rs_copy(layer, 1, t3).wait_send()
        rs_copy(layer, 2, t1).wait_send()
        return 0

    lax.fori_loop(0, LAYERS, drain, 0)


def fused(tokens_in, norm_gain, w_pool_in, w_gate, w_back):
    sp_count, tp_count = lax.axis_size("sp"), lax.axis_size("tp")
    toks, feats = tokens_in.shape
    _, depth, local_pool = w_pool_in.shape
    rounds = sp_count - 1
    bf, f32 = jnp.bfloat16, jnp.float32
    dma = pltpu.SemaphoreType.DMA
    streams = dma((LAYERS, 2, rounds, 3))
    return pl.pallas_call(
        functools.partial(fused_kernel, sp_count, tp_count),
        out_shape=jax.ShapeDtypeStruct((toks, feats), bf),
        in_specs=[
            pl.BlockSpec(memory_space=pltpu.HBM),
            pl.BlockSpec(memory_space=pltpu.VMEM),
            pl.BlockSpec(memory_space=pltpu.HBM),
            pl.BlockSpec(memory_space=pltpu.HBM),
            pl.BlockSpec(memory_space=pltpu.HBM),
        ],
        out_specs=pl.BlockSpec(memory_space=pltpu.VMEM),
        scratch_shapes=[
            pltpu.VMEM((LAYERS, sp_count) + w_pool_in.shape[1:], bf),
            pltpu.VMEM((LAYERS, sp_count) + w_gate.shape[1:], bf),
            pltpu.VMEM((LAYERS, sp_count) + w_back.shape[1:], bf),
            pltpu.VMEM((LAYERS, tp_count, toks, feats), bf),
            pltpu.VMEM((toks, tp_count * feats), bf),
            pltpu.VMEM((LAYERS, 3, toks, local_pool), bf),
            pltpu.VMEM((toks, feats), f32),
            pltpu.VMEM((3, toks, toks), bf),
            pltpu.VMEM((toks, local_pool), f32),
            pltpu.VMEM((LAYERS, tp_count, toks, feats), bf),
            pltpu.VMEM((LAYERS, 3, toks, feats), bf),
            dma((LAYERS + 1, 3)),
            streams, streams, streams, streams,
            dma((LAYERS, 3)), dma((LAYERS, 3)),
            dma((LAYERS, 2)), dma((LAYERS, 2)),
            dma((LAYERS, 3)), dma((LAYERS, 3)),
        ],
        compiler_params=pltpu.CompilerParams(
            collective_id=0, has_side_effects=True, vmem_limit_bytes=56 * 1024 * 1024
        ),
    )(tokens_in, norm_gain, w_pool_in, w_gate, w_back)


def dispatch(tokens_in, norm_gain, w_pool_in, w_gate, w_back):
    fits = (
        lax.axis_size("grp") == 2
        and lax.axis_size("tp") == GROUPS == 4
        and lax.axis_size("sp") == lax.axis_size("tp")
        and w_pool_in.shape[2] * GROUPS == POOL_WIDTH
        and w_pool_in.shape[1] == tokens_in.shape[1]
        and tokens_in.shape[0] // GRID_W >= max(pool_windows) // 2
    )
    step = fused if fits else on_device
    return step(tokens_in, norm_gain, w_pool_in, w_gate, w_back)


def solution(mesh):
    return jax.shard_map(
        dispatch,
        mesh=mesh,
        in_specs=(
            P(("grp", "sp"), "tp"),
            P(),
            P(None, "sp", "tp"),
            P(None, "sp", "tp"),
            P(None, "tp", "sp"),
        ),
        out_specs=P(("grp", "sp"), "tp"),
        check_vma=False,
    )
```

```python
import jax
import jax.numpy as jnp
from jax import lax
from jax.experimental import pallas as pl
from jax.experimental.pallas import tpu as pltpu
from jax.sharding import PartitionSpec as P
import functools

POOL_WIDTH = 1024
GROUPS = 4
GRID_W = 32
LAYERS = 3


pool_windows = (2, 4, 8, 16)
norm_eps = 1e-06


def padded_2(value, sides, width):
    for axis, dim in sides:
        peers, length = (lax.axis_size(axis), value.shape[dim])
        up = [(i, (i + 1) % peers) for i in range(peers - 1)]
        down = [(j, i) for i, j in up]
        last = lax.slice_in_dim(value, length - width, length, axis=dim)
        initial = lax.slice_in_dim(value, 0, width, axis=dim)
        before = lax.ppermute(last, axis, up)
        after = lax.ppermute(initial, axis, down)
        value = jnp.concatenate([before, value, after], axis=dim)
    return value


def window_means(padded, rows_here, first_row, total_rows, window):
    reach = max(pool_windows) // 2
    half_span = window // 2
    width_cols = padded.shape[1] - 2 * reach
    row_sums = padded[reach - half_span : reach - half_span + rows_here]
    for offset in range(1 - half_span, half_span):
        row_sums = row_sums + padded[reach + offset : reach + offset + rows_here]
    box_sums = row_sums[:, reach - half_span : reach - half_span + width_cols]
    for offset in range(1 - half_span, half_span):
        box_sums = box_sums + row_sums[:, reach + offset : reach + offset + width_cols]
    row_index = first_row + jnp.arange(rows_here, dtype=jnp.int32)
    col_index = jnp.arange(width_cols, dtype=jnp.int32)
    row_counts = jnp.minimum(row_index + half_span, total_rows) - jnp.maximum(
        row_index - half_span, 0
    )
    col_counts = jnp.minimum(col_index + half_span, width_cols) - jnp.maximum(
        col_index - half_span, 0
    )
    counts = (row_counts[:, None] * col_counts[None, :]).astype(jnp.float32)
    return box_sums / counts[:, :, None]


def on_device(tokens_in, norm_gain, w_pool_in, w_gate, w_back):
    reach = max(pool_windows) // 2
    sp_count = lax.axis_size("sp")
    tp_count = lax.axis_size("tp")
    tp_pos = lax.axis_index("tp")
    sp_pos = lax.axis_index("sp")
    tok_rows = tokens_in.shape[0]
    rows_here = tok_rows // GRID_W
    total_rows = rows_here * sp_count
    first_row = sp_pos * rows_here
    local_pool = w_pool_in.shape[2]
    group_width = POOL_WIDTH // GROUPS
    channel_group = (tp_pos * local_pool + jnp.arange(local_pool, dtype=jnp.int32)) // group_width
    state = tokens_in
    for layer_id in range(LAYERS):
        whole_rows = lax.all_gather(state, "tp", axis=1, tiled=True)
        wide = whole_rows.astype(jnp.float32)
        normed = (
            wide
            * lax.rsqrt(jnp.mean(wide * wide, axis=-1, keepdims=True) + norm_eps)
            * norm_gain[layer_id]
        ).astype(jnp.bfloat16)
        pool_acc = jnp.dot(
            normed,
            lax.all_gather(w_pool_in[layer_id], "sp", axis=0, tiled=True),
            preferred_element_type=jnp.float32,
        )
        gate_acc = jnp.dot(
            normed,
            lax.all_gather(w_gate[layer_id], "sp", axis=0, tiled=True),
            preferred_element_type=jnp.float32,
        )
        pool_in = pool_acc.astype(jnp.bfloat16)
        gate = jax.nn.sigmoid(gate_acc)
        cells = pool_in.reshape(rows_here, GRID_W, local_pool)
        rimmed = padded_2(cells, (("sp", 0),), reach)
        padded = jnp.pad(rimmed.astype(jnp.float32), ((0, 0), (reach, reach), (0, 0)))
        means = jnp.zeros((rows_here, GRID_W, local_pool), jnp.float32)
        for group_id in range(GROUPS):
            in_group = (channel_group == group_id)[None, None, :]
            means = jnp.where(
                in_group,
                window_means(padded, rows_here, first_row, total_rows, pool_windows[group_id]),
                means,
            )
        pooled = (
            (means - cells.astype(jnp.float32)).reshape(tok_rows, local_pool).astype(jnp.bfloat16)
        )
        full_pooled = lax.all_gather(pooled, "tp", axis=1, tiled=True)
        back_rows = lax.all_gather(w_back[layer_id], "sp", axis=1, tiled=True)
        back_cols = lax.all_to_all(back_rows, "tp", split_axis=1, concat_axis=0, tiled=True)
        partials = jnp.einsum(
            "tnb,nbd->ntd",
            full_pooled.reshape(tok_rows, tp_count, local_pool),
            back_cols.reshape(tp_count, local_pool, back_cols.shape[1]),
            preferred_element_type=jnp.float32,
        ).astype(jnp.bfloat16)
        branch = jnp.sum(partials.astype(jnp.float32), axis=0)
        state = (state.astype(jnp.float32) + gate * branch).astype(jnp.bfloat16)
    return state


MESH = pl.DeviceIdType.MESH
POOL, GATE, BACK = range(3)


def halves(buffers, layer, block, half):
    views = []
    for buf in buffers:
        rows = buf.shape[2] // 2
        views.append(buf.at[layer, block, pl.ds(pl.multiple_of(half * rows, rows), rows), :])
    return views


def fused_kernel(
    sp_count, tp_count,
    tok_hbm, gain_ref, wp_hbm, wg_hbm, wb_hbm, out_ref,
    wp, wg, wb, gathered, normed, halo, gate_buf, box, counts, parts, arrived,
    load_sem, z_send, z_recv, y_send, y_recv, ag_send, ag_recv, h_send, h_recv, rs_send, rs_recv,
):
    g = lax.axis_index("grp")
    s = lax.axis_index("sp")
    t = lax.axis_index("tp")
    other = 1 - g
    t1 = t + 1 - 2 * (t % 2)
    t2 = (t + 2) % tp_count
    t3 = (t1 + 2) % tp_count
    last = sp_count - 1
    toks, feats = tok_hbm.shape
    rows_here = toks // GRID_W
    total_rows = rows_here * sp_count
    weights = (wp, wg, wb)
    sources = (wp_hbm, wg_hbm, wb_hbm)
    rounds = sp_count - 1

    def load(layer, piece):
        return pltpu.make_async_copy(
            sources[piece].at[layer], weights[piece].at[layer, s], load_sem.at[layer, piece]
        )

    state_load = pltpu.make_async_copy(tok_hbm, gathered.at[0, t], load_sem.at[LAYERS, 0])
    state_load.start()
    for piece in range(3):
        load(0, piece).start()
    for layer in range(1, LAYERS):
        for piece in range(3):
            load(layer, piece).start()

    barrier = pltpu.get_barrier_semaphore()
    for target in ({"grp": other}, {"tp": t1}, {"tp": t2}, {"tp": t3}):
        pl.semaphore_signal(barrier, inc=1, device_id=target, device_id_type=MESH)

    @pl.when(s > 0)
    def _():
        pl.semaphore_signal(barrier, inc=1, device_id={"sp": s - 1}, device_id_type=MESH)

    @pl.when(s < last)
    def _():
        pl.semaphore_signal(barrier, inc=1, device_id={"sp": s + 1}, device_id_type=MESH)

    pl.semaphore_wait(barrier, 4 + jnp.where(s > 0, 1, 0) + jnp.where(s < last, 1, 0))

    def sent_block(way, k):
        return s - k if way == 0 else s + k

    def got_block(way, k):
        return s - 1 - k if way == 0 else s + 1 + k

    def gets(way, k):
        return s - 1 - k >= 0 if way == 0 else s + 1 + k <= last

    def sends(way, k):
        if way == 0:
            return jnp.logical_and(s - k >= 0, s < last)
        return jnp.logical_and(s + k <= last, s > 0)

    def z_copy(layer, way, k, piece, block):
        view = halves(weights, layer, block, g)[piece]
        return pltpu.make_async_remote_copy(
            src_ref=view, dst_ref=view,
            send_sem=z_send.at[layer, way, k, piece], recv_sem=z_recv.at[layer, way, k, piece],
            device_id={"sp": s + 1 if way == 0 else s - 1}, device_id_type=MESH,
        )

    def y_copy(layer, way, k, piece, half):
        view = halves(weights, layer, got_block(way, k), half)[piece]
        return pltpu.make_async_remote_copy(
            src_ref=view, dst_ref=view,
            send_sem=y_send.at[layer, way, k, piece], recv_sem=y_recv.at[layer, way, k, piece],
            device_id={"grp": other}, device_id_type=MESH,
        )

    def own_sends(layer, piece):
        load(layer, piece).wait()
        for way in range(2):
            @pl.when(sends(way, 0))
            def _(way=way):
                z_copy(layer, way, 0, piece, s).start()

    def pump(layer, piece, k):
        for way in range(2):
            @pl.when(gets(way, k))
            def _(way=way):
                z_copy(layer, way, k, piece, got_block(way, k)).wait_recv()
                y_copy(layer, way, k, piece, g).start()
            if k + 1 < rounds:
                @pl.when(sends(way, k + 1))
                def _(way=way):
                    z_copy(layer, way, k + 1, piece, sent_block(way, k + 1)).start()

    def await_y(layer, piece):
        for k in range(rounds):
            for way in range(2):
                @pl.when(gets(way, k))
                def _(way=way, k=k):
                    y_copy(layer, way, k, piece, other).wait_recv()

    def ag_copy(layer, which, block, target):
        return pltpu.make_async_remote_copy(
            src_ref=gathered.at[layer, block], dst_ref=gathered.at[layer, block],
            send_sem=ag_send.at[layer, which], recv_sem=ag_recv.at[layer, which],
            device_id={"tp": target}, device_id_type=MESH,
        )

    def start_gather(layer):
        ag_copy(layer, 0, t, t2).start()
        ag_copy(layer, 1, t, t1).start()

    def h_copy(layer, way):
        return pltpu.make_async_remote_copy(
            src_ref=halo.at[layer, 1], dst_ref=halo.at[layer, 0 if way == 0 else 2],
            send_sem=h_send.at[layer, way], recv_sem=h_recv.at[layer, way],
            device_id={"sp": s + 1 if way == 0 else s - 1}, device_id_type=MESH,
        )

    def rs_copy(layer, which, target):
        return pltpu.make_async_remote_copy(
            src_ref=parts.at[layer, target], dst_ref=arrived.at[layer, which],
            send_sem=rs_send.at[layer, which], recv_sem=rs_recv.at[layer, which],
            device_id={"tp": target}, device_id_type=MESH,
        )

    state_load.wait()
    start_gather(0)
    own_sends(0, POOL)
    own_sends(0, BACK)

    half_span = jnp.int32(pool_windows[0] // 2)
    for group_id in range(1, GROUPS):
        half_span = jnp.where(t == group_id, pool_windows[group_id] // 2, half_span)
    shift = GRID_W.bit_length() - 1
    first_row = s * rows_here
    out_tok = lax.broadcasted_iota(jnp.int32, (toks, toks), 0)
    in_tok = lax.broadcasted_iota(jnp.int32, (toks, toks), 1)
    out_row = first_row + lax.shift_right_logical(out_tok, shift)
    out_col = lax.bitwise_and(out_tok, GRID_W - 1)
    in_col = lax.bitwise_and(in_tok, GRID_W - 1)
    near_col = (in_col >= out_col - half_span) & (in_col < out_col + half_span)
    for slot in range(3):
        in_row = first_row + (slot - 1) * rows_here + lax.shift_right_logical(in_tok, shift)
        inside = (
            near_col
            & (in_row >= out_row - half_span) & (in_row < out_row + half_span)
            & (in_row >= 0) & (in_row < total_rows)
        )
        box[slot] = jnp.where(inside, 1.0, 0.0).astype(jnp.bfloat16)
    tok_at = lax.broadcasted_iota(jnp.int32, counts.shape, 0)
    row_at = first_row + lax.shift_right_logical(tok_at, shift)
    col_at = lax.bitwise_and(tok_at, GRID_W - 1)
    row_counts = jnp.minimum(row_at + half_span, total_rows) - jnp.maximum(row_at - half_span, 0)
    col_counts = jnp.minimum(col_at + half_span, GRID_W) - jnp.maximum(col_at - half_span, 0)
    counts[...] = (row_counts * col_counts).astype(jnp.float32)

    @pl.when(s == 0)
    def _():
        for layer in range(LAYERS):
            halo[layer, 0] = jnp.zeros(halo.shape[2:], halo.dtype)

    @pl.when(s == last)
    def _():
        for layer in range(LAYERS):
            halo[layer, 2] = jnp.zeros(halo.shape[2:], halo.dtype)

    for k in range(rounds):
        pump(0, POOL, k)

    def one_layer(layer, _):
        more = layer + 1 < LAYERS

        pump(layer, BACK, 0)
        own_sends(layer, GATE)
        ag_copy(layer, 0, t2, t2).wait_recv()
        ag_copy(layer, 2, t2, t1).start()
        ag_copy(layer, 1, t1, t1).wait_recv()
        ag_copy(layer, 2, t3, t1).wait_recv()
        total = jnp.zeros((toks, 1), jnp.float32)
        for block in range(tp_count):
            wide = gathered[layer, block].astype(jnp.float32)
            total = total + jnp.sum(wide * wide, axis=1, keepdims=True)
        scale = lax.rsqrt(total / (tp_count * feats) + norm_eps)
        for block in range(tp_count):
            cols = slice(block * feats, (block + 1) * feats)
            wide = gathered[layer, block].astype(jnp.float32)
            normed[:, cols] = (wide * scale * gain_ref[pl.ds(layer, 1), cols]).astype(jnp.bfloat16)

        for k in range(1, rounds - 1):
            pump(layer, BACK, k)
        depth = wp.shape[2]

        def project(buf):
            acc = None
            for block in range(sp_count):
                term = jnp.dot(
                    normed[:, block * depth:(block + 1) * depth], buf[layer, block],
                    preferred_element_type=jnp.float32,
                )
                acc = term if acc is None else acc + term
            return acc

        await_y(layer, POOL)
        halo[layer, 1] = project(wp).astype(jnp.bfloat16)

        @pl.when(s < last)
        def _():
            h_copy(layer, 0).start()

        @pl.when(s > 0)
        def _():
            h_copy(layer, 1).start()

        pump(layer, BACK, rounds - 1)

        pump(layer, GATE, 0)

        @pl.when(more)
        def _():
            own_sends(layer + 1, POOL)


        @pl.when(s > 0)
        def _():
            h_copy(layer, 0).wait_recv()

        @pl.when(s < last)
        def _():
            h_copy(layer, 1).wait_recv()

        sums = jnp.zeros(counts.shape, jnp.float32)
        for slot in range(3):
            sums = sums + jnp.dot(box[slot], halo[layer, slot], preferred_element_type=jnp.float32)
        pooled = (sums / counts[...] - halo[layer, 1].astype(jnp.float32)).astype(jnp.bfloat16)
        await_y(layer, BACK)
        for which, target in ((1, t3), (0, t2), (2, t1), (None, t)):
            parts[layer, target] = jnp.dot(
                pooled, wb[layer, target], preferred_element_type=jnp.float32
            ).astype(jnp.bfloat16)
            if which is not None:
                rs_copy(layer, which, target).start()

        for k in range(1, rounds):
            pump(layer, GATE, k)

        @pl.when(more)
        def _():
            pump(layer + 1, POOL, 0)
            own_sends(layer + 1, BACK)
            for k in range(1, rounds - 1):
                pump(layer + 1, POOL, k)

        await_y(layer, GATE)
        gate_buf[...] = jax.nn.sigmoid(project(wg))
        branch = parts[layer, t].astype(jnp.float32)
        for which in (2, 0, 1):
            rs_copy(layer, which, t1).wait_recv()
            branch = branch + arrived[layer, which].astype(jnp.float32)
        state = (gathered[layer, t].astype(jnp.float32) + gate_buf[...] * branch).astype(jnp.bfloat16)

        @pl.when(more)
        def _():
            gathered[layer + 1, t] = state
            start_gather(layer + 1)
            pump(layer + 1, POOL, rounds - 1)

        @pl.when(layer + 1 == LAYERS)
        def _():
            out_ref[...] = state

        return 0

    lax.fori_loop(0, LAYERS, one_layer, 0)

    def drain(layer, _):
        for piece in range(3):
            for k in range(rounds):
                for way in range(2):
                    @pl.when(sends(way, k))
                    def _(way=way, k=k, piece=piece):
                        z_copy(layer, way, k, piece, sent_block(way, k)).wait_send()

                    @pl.when(gets(way, k))
                    def _(way=way, k=k, piece=piece):
                        y_copy(layer, way, k, piece, g).wait_send()
        ag_copy(layer, 0, t, t2).wait_send()
        ag_copy(layer, 1, t, t1).wait_send()
        ag_copy(layer, 2, t2, t1).wait_send()

        @pl.when(s < last)
        def _():
            h_copy(layer, 0).wait_send()

        @pl.when(s > 0)
        def _():
            h_copy(layer, 1).wait_send()

        rs_copy(layer, 0, t2).wait_send()
        rs_copy(layer, 1, t3).wait_send()
        rs_copy(layer, 2, t1).wait_send()
        return 0

    lax.fori_loop(0, LAYERS, drain, 0)


def fused(tokens_in, norm_gain, w_pool_in, w_gate, w_back):
    sp_count, tp_count = lax.axis_size("sp"), lax.axis_size("tp")
    toks, feats = tokens_in.shape
    _, depth, local_pool = w_pool_in.shape
    rounds = sp_count - 1
    bf, f32 = jnp.bfloat16, jnp.float32
    dma = pltpu.SemaphoreType.DMA
    streams = dma((LAYERS, 2, rounds, 3))
    return pl.pallas_call(
        functools.partial(fused_kernel, sp_count, tp_count),
        out_shape=jax.ShapeDtypeStruct((toks, feats), bf),
        in_specs=[
            pl.BlockSpec(memory_space=pltpu.HBM),
            pl.BlockSpec(memory_space=pltpu.VMEM),
            pl.BlockSpec(memory_space=pltpu.HBM),
            pl.BlockSpec(memory_space=pltpu.HBM),
            pl.BlockSpec(memory_space=pltpu.HBM),
        ],
        out_specs=pl.BlockSpec(memory_space=pltpu.VMEM),
        scratch_shapes=[
            pltpu.VMEM((LAYERS, sp_count) + w_pool_in.shape[1:], bf),
            pltpu.VMEM((LAYERS, sp_count) + w_gate.shape[1:], bf),
            pltpu.VMEM((LAYERS, sp_count) + w_back.shape[1:], bf),
            pltpu.VMEM((LAYERS, tp_count, toks, feats), bf),
            pltpu.VMEM((toks, tp_count * feats), bf),
            pltpu.VMEM((LAYERS, 3, toks, local_pool), bf),
            pltpu.VMEM((toks, feats), f32),
            pltpu.VMEM((3, toks, toks), bf),
            pltpu.VMEM((toks, local_pool), f32),
            pltpu.VMEM((LAYERS, tp_count, toks, feats), bf),
            pltpu.VMEM((LAYERS, 3, toks, feats), bf),
            dma((LAYERS + 1, 3)),
            streams, streams, streams, streams,
            dma((LAYERS, 3)), dma((LAYERS, 3)),
            dma((LAYERS, 2)), dma((LAYERS, 2)),
            dma((LAYERS, 3)), dma((LAYERS, 3)),
        ],
        compiler_params=pltpu.CompilerParams(
            collective_id=0, has_side_effects=True, vmem_limit_bytes=56 * 1024 * 1024
        ),
    )(tokens_in, norm_gain, w_pool_in, w_gate, w_back)


def dispatch(tokens_in, norm_gain, w_pool_in, w_gate, w_back):
    fits = (
        lax.axis_size("grp") == 2
        and lax.axis_size("tp") == GROUPS == 4
        and lax.axis_size("sp") == lax.axis_size("tp")
        and w_pool_in.shape[2] * GROUPS == POOL_WIDTH
        and w_pool_in.shape[1] == tokens_in.shape[1]
        and tokens_in.shape[0] // GRID_W >= max(pool_windows) // 2
    )
    step = fused if fits else on_device
    return step(tokens_in, norm_gain, w_pool_in, w_gate, w_back)


def solution(mesh):
    return jax.shard_map(
        dispatch,
        mesh=mesh,
        in_specs=(
            P(("grp", "sp"), "tp"),
            P(),
            P(None, "sp", "tp"),
            P(None, "sp", "tp"),
            P(None, "tp", "sp"),
        ),
        out_specs=P(("grp", "sp"), "tp"),
        check_vma=False,
    )
```

```python
import jax
import jax.numpy as jnp
from jax import lax
from jax.experimental import pallas as pl
from jax.experimental.pallas import tpu as pltpu
from jax.sharding import PartitionSpec as P
import functools

POOL_WIDTH = 1024
GROUPS = 4
GRID_W = 32
LAYERS = 3


pool_windows = (2, 4, 8, 16)
norm_eps = 1e-06


def padded_2(value, sides, width):
    for axis, dim in sides:
        peers, length = (lax.axis_size(axis), value.shape[dim])
        up = [(i, (i + 1) % peers) for i in range(peers - 1)]
        down = [(j, i) for i, j in up]
        last = lax.slice_in_dim(value, length - width, length, axis=dim)
        initial = lax.slice_in_dim(value, 0, width, axis=dim)
        before = lax.ppermute(last, axis, up)
        after = lax.ppermute(initial, axis, down)
        value = jnp.concatenate([before, value, after], axis=dim)
    return value


def window_means(padded, rows_here, first_row, total_rows, window):
    reach = max(pool_windows) // 2
    half_span = window // 2
    width_cols = padded.shape[1] - 2 * reach
    row_sums = padded[reach - half_span : reach - half_span + rows_here]
    for offset in range(1 - half_span, half_span):
        row_sums = row_sums + padded[reach + offset : reach + offset + rows_here]
    box_sums = row_sums[:, reach - half_span : reach - half_span + width_cols]
    for offset in range(1 - half_span, half_span):
        box_sums = box_sums + row_sums[:, reach + offset : reach + offset + width_cols]
    row_index = first_row + jnp.arange(rows_here, dtype=jnp.int32)
    col_index = jnp.arange(width_cols, dtype=jnp.int32)
    row_counts = jnp.minimum(row_index + half_span, total_rows) - jnp.maximum(
        row_index - half_span, 0
    )
    col_counts = jnp.minimum(col_index + half_span, width_cols) - jnp.maximum(
        col_index - half_span, 0
    )
    counts = (row_counts[:, None] * col_counts[None, :]).astype(jnp.float32)
    return box_sums / counts[:, :, None]


def on_device(tokens_in, norm_gain, w_pool_in, w_gate, w_back):
    reach = max(pool_windows) // 2
    sp_count = lax.axis_size("sp")
    tp_count = lax.axis_size("tp")
    tp_pos = lax.axis_index("tp")
    sp_pos = lax.axis_index("sp")
    tok_rows = tokens_in.shape[0]
    rows_here = tok_rows // GRID_W
    total_rows = rows_here * sp_count
    first_row = sp_pos * rows_here
    local_pool = w_pool_in.shape[2]
    group_width = POOL_WIDTH // GROUPS
    channel_group = (tp_pos * local_pool + jnp.arange(local_pool, dtype=jnp.int32)) // group_width
    state = tokens_in
    for layer_id in range(LAYERS):
        whole_rows = lax.all_gather(state, "tp", axis=1, tiled=True)
        wide = whole_rows.astype(jnp.float32)
        normed = (
            wide
            * lax.rsqrt(jnp.mean(wide * wide, axis=-1, keepdims=True) + norm_eps)
            * norm_gain[layer_id]
        ).astype(jnp.bfloat16)
        pool_acc = jnp.dot(
            normed,
            lax.all_gather(w_pool_in[layer_id], "sp", axis=0, tiled=True),
            preferred_element_type=jnp.float32,
        )
        gate_acc = jnp.dot(
            normed,
            lax.all_gather(w_gate[layer_id], "sp", axis=0, tiled=True),
            preferred_element_type=jnp.float32,
        )
        pool_in = pool_acc.astype(jnp.bfloat16)
        gate = jax.nn.sigmoid(gate_acc)
        cells = pool_in.reshape(rows_here, GRID_W, local_pool)
        rimmed = padded_2(cells, (("sp", 0),), reach)
        padded = jnp.pad(rimmed.astype(jnp.float32), ((0, 0), (reach, reach), (0, 0)))
        means = jnp.zeros((rows_here, GRID_W, local_pool), jnp.float32)
        for group_id in range(GROUPS):
            in_group = (channel_group == group_id)[None, None, :]
            means = jnp.where(
                in_group,
                window_means(padded, rows_here, first_row, total_rows, pool_windows[group_id]),
                means,
            )
        pooled = (
            (means - cells.astype(jnp.float32)).reshape(tok_rows, local_pool).astype(jnp.bfloat16)
        )
        full_pooled = lax.all_gather(pooled, "tp", axis=1, tiled=True)
        back_rows = lax.all_gather(w_back[layer_id], "sp", axis=1, tiled=True)
        back_cols = lax.all_to_all(back_rows, "tp", split_axis=1, concat_axis=0, tiled=True)
        partials = jnp.einsum(
            "tnb,nbd->ntd",
            full_pooled.reshape(tok_rows, tp_count, local_pool),
            back_cols.reshape(tp_count, local_pool, back_cols.shape[1]),
            preferred_element_type=jnp.float32,
        ).astype(jnp.bfloat16)
        branch = jnp.sum(partials.astype(jnp.float32), axis=0)
        state = (state.astype(jnp.float32) + gate * branch).astype(jnp.bfloat16)
    return state


MESH = pl.DeviceIdType.MESH
POOL, GATE, BACK = range(3)


def halves(buffers, layer, block, half):
    views = []
    for buf in buffers:
        rows = buf.shape[2] // 2
        views.append(buf.at[layer, block, pl.ds(pl.multiple_of(half * rows, rows), rows), :])
    return views


def fused_kernel(
    sp_count, tp_count,
    tok_hbm, gain_ref, wp_hbm, wg_hbm, wb_hbm, out_ref,
    wp, wg, wb, gathered, normed, halo, gate_buf, box, counts, parts, arrived,
    load_sem, z_send, z_recv, y_send, y_recv, ag_send, ag_recv, h_send, h_recv, rs_send, rs_recv,
):
    g = lax.axis_index("grp")
    s = lax.axis_index("sp")
    t = lax.axis_index("tp")
    other = 1 - g
    t1 = t + 1 - 2 * (t % 2)
    t2 = (t + 2) % tp_count
    t3 = (t1 + 2) % tp_count
    last = sp_count - 1
    toks, feats = tok_hbm.shape
    rows_here = toks // GRID_W
    total_rows = rows_here * sp_count
    weights = (wp, wg, wb)
    sources = (wp_hbm, wg_hbm, wb_hbm)
    rounds = sp_count - 1

    def load(layer, piece):
        return pltpu.make_async_copy(
            sources[piece].at[layer], weights[piece].at[layer, s], load_sem.at[layer, piece]
        )

    state_load = pltpu.make_async_copy(tok_hbm, gathered.at[0, t], load_sem.at[LAYERS, 0])
    state_load.start()
    for piece in range(3):
        load(0, piece).start()
    for layer in range(1, LAYERS):
        for piece in range(3):
            load(layer, piece).start()

    barrier = pltpu.get_barrier_semaphore()
    for target in ({"grp": other}, {"tp": t1}, {"tp": t2}, {"tp": t3}):
        pl.semaphore_signal(barrier, inc=1, device_id=target, device_id_type=MESH)

    @pl.when(s > 0)
    def _():
        pl.semaphore_signal(barrier, inc=1, device_id={"sp": s - 1}, device_id_type=MESH)

    @pl.when(s < last)
    def _():
        pl.semaphore_signal(barrier, inc=1, device_id={"sp": s + 1}, device_id_type=MESH)

    pl.semaphore_wait(barrier, 4 + jnp.where(s > 0, 1, 0) + jnp.where(s < last, 1, 0))

    def sent_block(way, k):
        return s - k if way == 0 else s + k

    def got_block(way, k):
        return s - 1 - k if way == 0 else s + 1 + k

    def gets(way, k):
        return s - 1 - k >= 0 if way == 0 else s + 1 + k <= last

    def sends(way, k):
        if way == 0:
            return jnp.logical_and(s - k >= 0, s < last)
        return jnp.logical_and(s + k <= last, s > 0)

    def z_copy(layer, way, k, piece, block):
        view = halves(weights, layer, block, g)[piece]
        return pltpu.make_async_remote_copy(
            src_ref=view, dst_ref=view,
            send_sem=z_send.at[layer, way, k, piece], recv_sem=z_recv.at[layer, way, k, piece],
            device_id={"sp": s + 1 if way == 0 else s - 1}, device_id_type=MESH,
        )

    def y_copy(layer, way, k, piece, half):
        view = halves(weights, layer, got_block(way, k), half)[piece]
        return pltpu.make_async_remote_copy(
            src_ref=view, dst_ref=view,
            send_sem=y_send.at[layer, way, k, piece], recv_sem=y_recv.at[layer, way, k, piece],
            device_id={"grp": other}, device_id_type=MESH,
        )

    def own_sends(layer, piece):
        load(layer, piece).wait()
        for way in range(2):
            @pl.when(sends(way, 0))
            def _(way=way):
                z_copy(layer, way, 0, piece, s).start()

    def pump(layer, piece, k):
        for way in range(2):
            @pl.when(gets(way, k))
            def _(way=way):
                z_copy(layer, way, k, piece, got_block(way, k)).wait_recv()
                y_copy(layer, way, k, piece, g).start()
            if k + 1 < rounds:
                @pl.when(sends(way, k + 1))
                def _(way=way):
                    z_copy(layer, way, k + 1, piece, sent_block(way, k + 1)).start()

    def await_y(layer, piece):
        for k in range(rounds):
            for way in range(2):
                @pl.when(gets(way, k))
                def _(way=way, k=k):
                    y_copy(layer, way, k, piece, other).wait_recv()

    def ag_copy(layer, which, block, target):
        return pltpu.make_async_remote_copy(
            src_ref=gathered.at[layer, block], dst_ref=gathered.at[layer, block],
            send_sem=ag_send.at[layer, which], recv_sem=ag_recv.at[layer, which],
            device_id={"tp": target}, device_id_type=MESH,
        )

    def start_gather(layer):
        ag_copy(layer, 0, t, t2).start()
        ag_copy(layer, 1, t, t1).start()

    def h_copy(layer, way):
        return pltpu.make_async_remote_copy(
            src_ref=halo.at[layer, 1], dst_ref=halo.at[layer, 0 if way == 0 else 2],
            send_sem=h_send.at[layer, way], recv_sem=h_recv.at[layer, way],
            device_id={"sp": s + 1 if way == 0 else s - 1}, device_id_type=MESH,
        )

    def rs_copy(layer, which, target):
        return pltpu.make_async_remote_copy(
            src_ref=parts.at[layer, target], dst_ref=arrived.at[layer, which],
            send_sem=rs_send.at[layer, which], recv_sem=rs_recv.at[layer, which],
            device_id={"tp": target}, device_id_type=MESH,
        )

    state_load.wait()
    start_gather(0)
    own_sends(0, POOL)
    own_sends(0, BACK)

    half_span = jnp.int32(pool_windows[0] // 2)
    for group_id in range(1, GROUPS):
        half_span = jnp.where(t == group_id, pool_windows[group_id] // 2, half_span)
    shift = GRID_W.bit_length() - 1
    first_row = s * rows_here
    out_tok = lax.broadcasted_iota(jnp.int32, (toks, toks), 0)
    in_tok = lax.broadcasted_iota(jnp.int32, (toks, toks), 1)
    out_row = first_row + lax.shift_right_logical(out_tok, shift)
    out_col = lax.bitwise_and(out_tok, GRID_W - 1)
    in_col = lax.bitwise_and(in_tok, GRID_W - 1)
    near_col = (in_col >= out_col - half_span) & (in_col < out_col + half_span)
    for slot in range(3):
        in_row = first_row + (slot - 1) * rows_here + lax.shift_right_logical(in_tok, shift)
        inside = (
            near_col
            & (in_row >= out_row - half_span) & (in_row < out_row + half_span)
            & (in_row >= 0) & (in_row < total_rows)
        )
        box[slot] = jnp.where(inside, 1.0, 0.0).astype(jnp.bfloat16)
    tok_at = lax.broadcasted_iota(jnp.int32, counts.shape, 0)
    row_at = first_row + lax.shift_right_logical(tok_at, shift)
    col_at = lax.bitwise_and(tok_at, GRID_W - 1)
    row_counts = jnp.minimum(row_at + half_span, total_rows) - jnp.maximum(row_at - half_span, 0)
    col_counts = jnp.minimum(col_at + half_span, GRID_W) - jnp.maximum(col_at - half_span, 0)
    counts[...] = (row_counts * col_counts).astype(jnp.float32)

    @pl.when(s == 0)
    def _():
        for layer in range(LAYERS):
            halo[layer, 0] = jnp.zeros(halo.shape[2:], halo.dtype)

    @pl.when(s == last)
    def _():
        for layer in range(LAYERS):
            halo[layer, 2] = jnp.zeros(halo.shape[2:], halo.dtype)

    for k in range(rounds):
        pump(0, POOL, k)

    def one_layer(layer, _):
        more = layer + 1 < LAYERS

        pump(layer, BACK, 0)
        ag_copy(layer, 0, t2, t2).wait_recv()
        ag_copy(layer, 2, t2, t1).start()
        own_sends(layer, GATE)
        ag_copy(layer, 1, t1, t1).wait_recv()
        ag_copy(layer, 2, t3, t1).wait_recv()
        total = jnp.zeros((toks, 1), jnp.float32)
        for block in range(tp_count):
            wide = gathered[layer, block].astype(jnp.float32)
            total = total + jnp.sum(wide * wide, axis=1, keepdims=True)
        scale = lax.rsqrt(total / (tp_count * feats) + norm_eps)
        for block in range(tp_count):
            cols = slice(block * feats, (block + 1) * feats)
            wide = gathered[layer, block].astype(jnp.float32)
            normed[:, cols] = (wide * scale * gain_ref[pl.ds(layer, 1), cols]).astype(jnp.bfloat16)

        for k in range(1, rounds - 1):
            pump(layer, BACK, k)
        depth = wp.shape[2]

        def project(buf):
            acc = None
            for block in range(sp_count):
                term = jnp.dot(
                    normed[:, block * depth:(block + 1) * depth], buf[layer, block],
                    preferred_element_type=jnp.float32,
                )
                acc = term if acc is None else acc + term
            return acc

        await_y(layer, POOL)
        halo[layer, 1] = project(wp).astype(jnp.bfloat16)

        @pl.when(s < last)
        def _():
            h_copy(layer, 0).start()

        @pl.when(s > 0)
        def _():
            h_copy(layer, 1).start()

        pump(layer, BACK, rounds - 1)

        pump(layer, GATE, 0)

        @pl.when(more)
        def _():
            own_sends(layer + 1, POOL)


        @pl.when(s > 0)
        def _():
            h_copy(layer, 0).wait_recv()

        @pl.when(s < last)
        def _():
            h_copy(layer, 1).wait_recv()

        sums = jnp.zeros(counts.shape, jnp.float32)
        for slot in range(3):
            sums = sums + jnp.dot(box[slot], halo[layer, slot], preferred_element_type=jnp.float32)
        pooled = (sums / counts[...] - halo[layer, 1].astype(jnp.float32)).astype(jnp.bfloat16)
        pump(layer, GATE, 1)
        await_y(layer, BACK)
        for which, target in ((1, t3), (0, t2), (2, t1), (None, t)):
            parts[layer, target] = jnp.dot(
                pooled, wb[layer, target], preferred_element_type=jnp.float32
            ).astype(jnp.bfloat16)
            if which is not None:
                rs_copy(layer, which, target).start()

        for k in range(2, rounds):
            pump(layer, GATE, k)

        @pl.when(more)
        def _():
            pump(layer + 1, POOL, 0)
            own_sends(layer + 1, BACK)
            for k in range(1, rounds - 1):
                pump(layer + 1, POOL, k)

        await_y(layer, GATE)
        gate_buf[...] = jax.nn.sigmoid(project(wg))
        branch = parts[layer, t].astype(jnp.float32)
        for which in (2, 0, 1):
            rs_copy(layer, which, t1).wait_recv()
            branch = branch + arrived[layer, which].astype(jnp.float32)
        state = (gathered[layer, t].astype(jnp.float32) + gate_buf[...] * branch).astype(jnp.bfloat16)

        @pl.when(more)
        def _():
            gathered[layer + 1, t] = state
            start_gather(layer + 1)
            pump(layer + 1, POOL, rounds - 1)

        @pl.when(layer + 1 == LAYERS)
        def _():
            out_ref[...] = state

        return 0

    lax.fori_loop(0, LAYERS, one_layer, 0)

    def drain(layer, _):
        for piece in range(3):
            for k in range(rounds):
                for way in range(2):
                    @pl.when(sends(way, k))
                    def _(way=way, k=k, piece=piece):
                        z_copy(layer, way, k, piece, sent_block(way, k)).wait_send()

                    @pl.when(gets(way, k))
                    def _(way=way, k=k, piece=piece):
                        y_copy(layer, way, k, piece, g).wait_send()
        ag_copy(layer, 0, t, t2).wait_send()
        ag_copy(layer, 1, t, t1).wait_send()
        ag_copy(layer, 2, t2, t1).wait_send()

        @pl.when(s < last)
        def _():
            h_copy(layer, 0).wait_send()

        @pl.when(s > 0)
        def _():
            h_copy(layer, 1).wait_send()

        rs_copy(layer, 0, t2).wait_send()
        rs_copy(layer, 1, t3).wait_send()
        rs_copy(layer, 2, t1).wait_send()
        return 0

    lax.fori_loop(0, LAYERS, drain, 0)


def fused(tokens_in, norm_gain, w_pool_in, w_gate, w_back):
    sp_count, tp_count = lax.axis_size("sp"), lax.axis_size("tp")
    toks, feats = tokens_in.shape
    _, depth, local_pool = w_pool_in.shape
    rounds = sp_count - 1
    bf, f32 = jnp.bfloat16, jnp.float32
    dma = pltpu.SemaphoreType.DMA
    streams = dma((LAYERS, 2, rounds, 3))
    return pl.pallas_call(
        functools.partial(fused_kernel, sp_count, tp_count),
        out_shape=jax.ShapeDtypeStruct((toks, feats), bf),
        in_specs=[
            pl.BlockSpec(memory_space=pltpu.HBM),
            pl.BlockSpec(memory_space=pltpu.VMEM),
            pl.BlockSpec(memory_space=pltpu.HBM),
            pl.BlockSpec(memory_space=pltpu.HBM),
            pl.BlockSpec(memory_space=pltpu.HBM),
        ],
        out_specs=pl.BlockSpec(memory_space=pltpu.VMEM),
        scratch_shapes=[
            pltpu.VMEM((LAYERS, sp_count) + w_pool_in.shape[1:], bf),
            pltpu.VMEM((LAYERS, sp_count) + w_gate.shape[1:], bf),
            pltpu.VMEM((LAYERS, sp_count) + w_back.shape[1:], bf),
            pltpu.VMEM((LAYERS, tp_count, toks, feats), bf),
            pltpu.VMEM((toks, tp_count * feats), bf),
            pltpu.VMEM((LAYERS, 3, toks, local_pool), bf),
            pltpu.VMEM((toks, feats), f32),
            pltpu.VMEM((3, toks, toks), bf),
            pltpu.VMEM((toks, local_pool), f32),
            pltpu.VMEM((LAYERS, tp_count, toks, feats), bf),
            pltpu.VMEM((LAYERS, 3, toks, feats), bf),
            dma((LAYERS + 1, 3)),
            streams, streams, streams, streams,
            dma((LAYERS, 3)), dma((LAYERS, 3)),
            dma((LAYERS, 2)), dma((LAYERS, 2)),
            dma((LAYERS, 3)), dma((LAYERS, 3)),
        ],
        compiler_params=pltpu.CompilerParams(
            collective_id=0, has_side_effects=True, vmem_limit_bytes=56 * 1024 * 1024
        ),
    )(tokens_in, norm_gain, w_pool_in, w_gate, w_back)


def dispatch(tokens_in, norm_gain, w_pool_in, w_gate, w_back):
    fits = (
        lax.axis_size("grp") == 2
        and lax.axis_size("tp") == GROUPS == 4
        and lax.axis_size("sp") == lax.axis_size("tp")
        and w_pool_in.shape[2] * GROUPS == POOL_WIDTH
        and w_pool_in.shape[1] == tokens_in.shape[1]
        and tokens_in.shape[0] // GRID_W >= max(pool_windows) // 2
    )
    step = fused if fits else on_device
    return step(tokens_in, norm_gain, w_pool_in, w_gate, w_back)


def solution(mesh):
    return jax.shard_map(
        dispatch,
        mesh=mesh,
        in_specs=(
            P(("grp", "sp"), "tp"),
            P(),
            P(None, "sp", "tp"),
            P(None, "sp", "tp"),
            P(None, "tp", "sp"),
        ),
        out_specs=P(("grp", "sp"), "tp"),
        check_vma=False,
    )
```
